32 devices in a mesh: grp: 2 (over y), ra: 4 (over z), cb: 4 (over x, core).
Axes of the slice: x: 2, y: 2, z: 4, core: 2. Of those that a mesh axis runs over, the one named last changes fastest.
Arguments:
- tokens: bfloat16 [256, 2048], P('grp', 'ra'), parts along dimension 0, may hold values from -8 to 8
- first_gain: bfloat16 [2048], P('ra'), may hold values from 0.099609375 to 1.8984375
- first_gate: bfloat16 [2048, 5632], P('ra', 'cb'), may hold values from -0.125 to 0.125
- first_up: bfloat16 [2048, 5632], P('ra', 'cb'), may hold values from -0.125 to 0.125
- first_down: bfloat16 [5632, 2048], P('cb', 'ra'), may hold values from -0.078125 to 0.078125
- second_gain: bfloat16 [2048], P('ra'), may hold values from 0.099609375 to 1.8984375
- second_gate: bfloat16 [2048, 5632], P('ra', 'cb'), may hold values from -0.125 to 0.125
- second_up: bfloat16 [2048, 5632], P('ra', 'cb'), may hold values from -0.125 to 0.125
- second_down: bfloat16 [5632, 2048], P('cb', 'ra'), may hold values from -0.078125 to 0.078125
Outputs:
- latent_out: bfloat16 [256, 2048], P('grp', 'ra'), parts along dimension 0
The draws below stay inside these ranges and needn't reach their ends.
There are 2 independent parts, one for each index of `grp`. The reference program is written for one: setup_inputs(seed, part) draws one part's arguments, and reference() takes and returns one part's arrays. A program takes and returns all parts, laid end to end along the dimension named above; an argument that names none is the same for every part. Nothing has to cross between parts.
All inputs are finite; a program needn't handle non-finite values.
Results may differ from the reference program's by a relative error of at most 0.0088.
Values may be sent and summed in bfloat16 or wider, within the bound.
A program may use at most 64 MiB of HBM per device.

```python
import math
import jax
import jax.numpy as jnp
from jax import lax

D = 2048
FF = 5632
TOKENS = 128


def draw_tokens(key, part):
    keys = jax.random.split(jax.random.fold_in(key, 11), 3)
    row_scale = jnp.exp(jax.random.uniform(keys[0], (TOKENS, 1), jnp.float32, math.log(0.1), 0.0))
    ramp = jnp.exp(math.log(6.0) * jnp.arange(D, dtype=jnp.float32) / D) / 2.5
    col_scale = ramp * jnp.exp(jax.random.uniform(keys[1], (D,), jnp.float32, -0.35, 0.35))
    base = jax.random.normal(keys[2], (TOKENS, D), jnp.float32)
    return jnp.clip(base * row_scale * col_scale, -8.0, 8.0).astype(jnp.bfloat16)


def steps_of(rng, dims, cuts, smallest, largest):
    def one(axis_at, shards_of):
        heights = jax.random.uniform(jax.random.fold_in(jax.random.fold_in(rng, 6), axis_at), (shards_of,), jnp.float32, smallest / len(cuts), largest / len(cuts))
        return jnp.repeat(jnp.exp(heights), dims[axis_at] // shards_of).reshape((-1,) + (1,) * (len(dims) - axis_at - 1))

    factor_of = one(*cuts[0])
    for cut in cuts[1:]:
        factor_of = factor_of * one(*cut)
    return factor_of


def centred(key, extent, deviation, bound, shards=(), kind=jnp.bfloat16):
    level = steps_of(key, extent, shards, -0.22, 0.18) if shards else 1.0
    result = jax.random.normal(key, extent, jnp.float32) * deviation * level
    return jnp.minimum(jnp.maximum(result, -bound), bound).astype(kind)


def setup_inputs(seed: int = 0, part: int = 0) -> dict:
    key_of = jax.random.split(jax.random.key(seed), 10)
    part_keys = jax.random.split(jax.random.fold_in(key_of[9], part), 10)
    tokens = draw_tokens(jax.random.fold_in(jax.random.fold_in(key_of[9], part), 71), part)
    first_gain = jnp.clip(1.0 + 0.18 * jax.random.normal(key_of[1], (D,), jnp.float32), 0.099609375, 1.8984375).astype(jnp.bfloat16)
    first_gate = centred(key_of[2], (D, FF), D ** -0.5, 0.125, ((0, 4), (1, 4)))
    first_up = centred(key_of[3], (D, FF), D ** -0.5, 0.125, ((0, 4), (1, 4)))
    first_down = centred(key_of[4], (FF, D), FF ** -0.5, 0.078125, ((0, 4), (1, 4)))
    second_gain = jnp.clip(1.0 + 0.18 * jax.random.normal(key_of[5], (D,), jnp.float32), 0.099609375, 1.8984375).astype(jnp.bfloat16)
    second_gate = centred(key_of[6], (D, FF), D ** -0.5, 0.125, ((0, 4), (1, 4)))
    second_up = centred(key_of[7], (D, FF), D ** -0.5, 0.125, ((0, 4), (1, 4)))
    second_down = centred(key_of[8], (FF, D), FF ** -0.5, 0.078125, ((0, 4), (1, 4)))
    return {"tokens": tokens, "first_gain": first_gain, "first_gate": first_gate, "first_up": first_up, "first_down": first_down, "second_gain": second_gain, "second_gate": second_gate, "second_up": second_up, "second_down": second_down}


def sublayer(x, gain, w_gate, w_up, w_down):
    xf = x.astype(jnp.float32)
    scale = jax.lax.rsqrt(lax.optimization_barrier(jnp.mean(xf * xf, axis=1)) + 1e-06)
    normed = (xf * gain.astype(jnp.float32)).astype(jnp.bfloat16)
    gate_pre = scale[:, None] * jnp.dot(normed, w_gate, preferred_element_type=jnp.float32)
    up_pre = scale[:, None] * jnp.dot(normed, w_up, preferred_element_type=jnp.float32)
    hidden = (jax.nn.silu(gate_pre) * up_pre).astype(jnp.bfloat16)
    branch = jnp.dot(hidden, w_down, preferred_element_type=jnp.float32)
    return (0.5 * xf + 0.5 * branch).astype(jnp.bfloat16)

def reference(tokens, first_gain, first_gate, first_up, first_down, second_gain, second_gate, second_up, second_down):
    middle = sublayer(tokens, first_gain, first_gate, first_up, first_down)
    return sublayer(middle, second_gain, second_gate, second_up, second_down)
```

```python
import functools

import jax
import jax.numpy as jnp
from jax import lax
from jax.experimental import pallas as pl
from jax.experimental.pallas import tpu as pltpu
from jax.sharding import PartitionSpec as P

MESH = pl.DeviceIdType.MESH
F32 = jnp.float32
BF16 = jnp.bfloat16
LAG = 4


def kernel(
    n, m, chunks, w, wp, pieces, half, width,
    x_ref, gain1, gate1, up1, down1, gain2, gate2, up2, down2, o_ref,
    xs, normed, wgu, wdn, send, recv, hid, sq_own, sq_in, sc, acc, r1, slots,
    w_sem, d_sem, send_sem, recv_sem, sq_send, sq_recv, dir_send, rel_send, hid_recv,
    core_send, core_recv, x_send, x_recv, mid_send, mid_recv,
):
    r = lax.axis_index("ra")
    b = lax.axis_index("cb")
    k0 = lax.rem(b, 2)
    xi = lax.div(b, 2)
    nx = m // 2
    sib = xi * 2 + 1 - k0
    odd = list(range(1, n, 2))
    cols = normed.shape[-1]
    pc = cols // pieces
    gains = (gain1, gain2)
    pos = (r, n - 1 - r)
    step = (1, -1)

    def place(d, p):
        return p if d == 0 else n - 1 - p

    def gate_copies(s, c):
        at = pl.ds(pl.multiple_of(c * w, w), w)
        g, u = ((gate1, up1), (gate2, up2))[s]
        return (
            pltpu.make_async_copy(g.at[:, at], wgu.at[s, c, :, pl.ds(0, w)], w_sem.at[s, c]),
            pltpu.make_async_copy(u.at[:, at], wgu.at[s, c, :, pl.ds(wp, w)], w_sem.at[s, c]),
        )

    def down_copy(s):
        return pltpu.make_async_copy((down1, down2)[s], wdn.at[s], d_sem.at[s])

    for s in range(2):
        @pl.loop(0, chunks)
        def _(c):
            for copy in gate_copies(s, c):
                copy.start()
        down_copy(s).start()

    barrier = pltpu.get_barrier_semaphore()
    for o in range(1, n):
        pl.semaphore_signal(barrier, 1, device_id={"ra": lax.rem(r + o, n)}, device_id_type=MESH)
    pl.semaphore_signal(barrier, 1, device_id={"cb": sib}, device_id_type=MESH)
    for o in range(1, nx):
        pl.semaphore_signal(
            barrier, 1, device_id={"cb": lax.rem(xi + o, nx) * 2 + k0}, device_id_type=MESH
        )

    for j in range(pieces):
        for d in range(2):
            xs[0, j, d] = x_ref[d * half:(d + 1) * half, j * pc:(j + 1) * pc]

    def remote(src, dst, ss, rs, where):
        return pltpu.make_async_remote_copy(
            src_ref=src, dst_ref=dst, send_sem=ss, recv_sem=rs, device_id=where, device_id_type=MESH
        )

    def sum_copy(s, d, c):
        return remote(send.at[s, d, c], recv.at[s, d, c], send_sem.at[s, d], recv_sem.at[s, d, c],
                      {"ra": r + step[d]})

    def hid_copy(s, d, c, ss, q):
        ref = hid.at[s, c, d]
        return remote(ref, ref, ss, hid_recv.at[s, d, c], {"ra": place(d, n - 1 - q)})

    def sq_copy(s, d, p):
        return remote(sq_own.at[s, d], sq_in.at[s, d, p], sq_send.at[s, d], sq_recv.at[s, d, p],
                      {"ra": place(d, n - 1)})

    def core_copy(s, j):
        return remote(acc.at[s, 1 - k0, j], r1.at[s, j], core_send.at[s, j], core_recv.at[s, j],
                      {"cb": sib})

    def x_copy(s, j, o):
        ref = slots.at[s, xi, j]
        return remote(ref, ref, x_send.at[s, o - 1, j], x_recv.at[s, o - 1, j],
                      {"cb": lax.rem(xi + o, nx) * 2 + k0})

    def mid_copy(s, j):
        ref = xs.at[s + 1, j, k0]
        return remote(ref, ref, mid_send.at[s, j], mid_recv.at[s, j], {"cb": sib})

    lane = lax.broadcasted_iota(jnp.int32, (8, 128), 1)
    for s in range(2):
        for d in range(2):
            total = jnp.zeros((half, 1), F32)
            for j in range(pieces):
                at = slice(j * pc, (j + 1) * pc)
                xf = xs[s, j, d].astype(F32)
                total = total + jnp.sum(xf * xf, axis=1, keepdims=True)
                normed[s, d, :, at] = (xf * gains[s][:, at].astype(F32)).astype(BF16)
            packed = jnp.zeros((8, 128), F32)
            for g in range(half // 8):
                packed = jnp.where(lane == g, total[g * 8:(g + 1) * 8], packed)
            sq_own[s, d] = packed
        if s == 0:
            pl.semaphore_wait(barrier, n - 1 + nx)
        for d in range(2):
            @pl.when(pos[d] < n - 1)
            def _():
                sq_copy(s, d, pos[d]).start()

        @pl.loop(0, chunks + LAG * n)
        def _(i):
            first = i - LAG * jnp.minimum(pos[0], pos[1])

            @pl.when((first >= 0) & (first < chunks))
            def _():
                whole = wgu.at[s, first, :, pl.ds(0, 2 * w)]
                pltpu.make_async_copy(whole, whole, w_sem.at[s, first]).wait()

            for d in range(2):
                c = i - LAG * pos[d]

                @pl.when((c >= 0) & (c < chunks))
                def _():
                    share = jnp.dot(normed[s, d], wgu[s, c], preferred_element_type=F32)

                    @pl.when(pos[d] == 0)
                    def _():
                        send[s, d, c] = share.astype(BF16)

                    @pl.when((pos[d] > 0) & (pos[d] < n - 1))
                    def _():
                        sum_copy(s, d, c).wait_recv()
                        send[s, d, c] = (share + recv[s, d, c].astype(F32)).astype(BF16)

                    @pl.when(pos[d] < n - 1)
                    def _():
                        sum_copy(s, d, c).start()

                    @pl.when(pos[d] == n - 1)
                    def _():
                        @pl.when(c == 0)
                        def _():
                            packed = sq_own[s, d]
                            for p in range(n - 1):
                                sq_copy(s, d, p).wait_recv()
                                packed = packed + sq_in[s, d, p]
                            packed = lax.rsqrt(packed / width + 1e-06)
                            for g in range(half // 8):
                                sc[s, d, g * 8:(g + 1) * 8] = jnp.broadcast_to(
                                    packed[:, g:g + 1], (8, 128)
                                )

                        sum_copy(s, d, c).wait_recv()
                        pre = share + recv[s, d, c].astype(F32)
                        scale = sc[s, d][:, :1]
                        gate = pre[:, :w] * scale
                        up = pre[:, wp:wp + w] * scale
                        hid[s, c, d] = (gate / (1.0 + jnp.exp(-gate)) * up).astype(BF16)
                        for t, q in enumerate(odd):
                            hid_copy(s, d, c, dir_send.at[s, d, t], q).start()

                back = n - 1 - pos[d]
                e = i - LAG * n

                @pl.when((lax.rem(back, 2) == 1) & (back < n - 1) & (e >= 0))
                def _():
                    hid_copy(s, d, e, rel_send.at[s, d], back + 1).wait_recv()
                    hid_copy(s, d, e, rel_send.at[s, d], back + 1).start()

        down_copy(s).wait()
        for j in range(pieces):
            for d in range(2):
                acc[s, d, j] = jnp.zeros((half, pc), F32)

        @pl.loop(0, chunks)
        def _(c):
            for d in range(2):
                back = n - 1 - pos[d]

                @pl.when((back > 0) & ((lax.rem(back, 2) == 0) | (back == n - 1)))
                def _():
                    hid_copy(s, d, c, rel_send.at[s, d], 1).wait_recv()

            rows = hid[s, c].reshape(2 * half, w)
            for j in range(pieces):
                out = jnp.dot(rows, wdn[s, c, :, j * pc:(j + 1) * pc], preferred_element_type=F32)
                for d in range(2):
                    acc[s, d, j] = acc[s, d, j] + out[d * half:(d + 1) * half]

        for j in range(pieces):
            core_copy(s, j).start()
        for j in range(pieces):
            core_copy(s, j).wait_recv()
            slots[s, xi, j] = (acc[s, k0, j] + r1[s, j]).astype(BF16)
            for o in range(1, nx):
                x_copy(s, j, o).start()
        for j in range(pieces):
            for o in range(1, nx):
                x_copy(s, j, o).wait_recv()
            branch = slots[s, 0, j].astype(F32)
            for o in range(1, nx):
                branch = branch + slots[s, o, j].astype(F32)
            xs[s + 1, j, k0] = (0.5 * xs[s, j, k0].astype(F32) + 0.5 * branch).astype(BF16)
            mid_copy(s, j).start()
        for j in range(pieces):
            mid_copy(s, j).wait_recv()

    for j in range(pieces):
        for d in range(2):
            o_ref[d * half:(d + 1) * half, j * pc:(j + 1) * pc] = xs[2, j, d]

    for s in range(2):
        for d in range(2):
            @pl.when(pos[d] < n - 1)
            def _():
                sq_copy(s, d, 0).wait_send()
                remote(send.at[s, d], recv.at[s, d], send_sem.at[s, d], recv_sem.at[s, d, 0],
                       {"ra": r + step[d]}).wait_send()

            ref = hid.at[s, :, d]

            @pl.when(pos[d] == n - 1)
            def _():
                for t, q in enumerate(odd):
                    remote(ref, ref, dir_send.at[s, d, t], hid_recv.at[s, d, 0],
                           {"ra": place(d, n - 1 - q)}).wait_send()

            back = n - 1 - pos[d]

            @pl.when((lax.rem(back, 2) == 1) & (back < n - 1))
            def _():
                remote(ref, ref, rel_send.at[s, d], hid_recv.at[s, d, 0],
                       {"ra": place(d, n - 2 - back)}).wait_send()

        for j in range(pieces):
            core_copy(s, j).wait_send()
            mid_copy(s, j).wait_send()
            for o in range(1, nx):
                x_copy(s, j, o).wait_send()


def per_device(n, m, x, gain1, gate1, up1, down1, gain2, gate2, up2, down2):
    rows, cols = x.shape
    ff = gate1.shape[1]
    w = wp = 128
    chunks = -(-ff // w)
    ragged = chunks * w - ff
    if ragged:
        gate1, up1, gate2, up2 = (
            jnp.pad(a, ((0, 0), (0, ragged))) for a in (gate1, up1, gate2, up2)
        )
        down1, down2 = (jnp.pad(a, ((0, ragged), (0, 0))) for a in (down1, down2))
    pieces = 2 if cols % 256 == 0 else 1
    half = rows // 2
    pc = cols // pieces
    odd = n // 2
    nx = m // 2
    vmem = pl.BlockSpec(memory_space=pltpu.VMEM)
    hbm = pl.BlockSpec(memory_space=pl.ANY)
    dma = pltpu.SemaphoreType.DMA
    return pl.pallas_call(
        functools.partial(kernel, n, m, chunks, w, wp, pieces, half, cols * n),
        out_shape=jax.ShapeDtypeStruct((rows, cols), BF16),
        in_specs=[vmem, vmem, hbm, hbm, hbm, vmem, hbm, hbm, hbm],
        out_specs=vmem,
        scratch_shapes=[
            pltpu.VMEM((3, pieces, 2, half, pc), BF16),
            pltpu.VMEM((2, 2, half, cols), BF16),
            pltpu.VMEM((2, chunks, cols, 2 * wp), BF16),
            pltpu.VMEM((2, chunks, w, cols), BF16),
            pltpu.VMEM((2, 2, chunks, half, 2 * wp), BF16),
            pltpu.VMEM((2, 2, chunks, half, 2 * wp), BF16),
            pltpu.VMEM((2, chunks, 2, half, w), BF16),
            pltpu.VMEM((2, 2, 8, 128), F32),
            pltpu.VMEM((2, 2, n, 8, 128), F32),
            pltpu.VMEM((2, 2, half, 128), F32),
            pltpu.VMEM((2, 2, pieces, half, pc), F32),
            pltpu.VMEM((2, pieces, half, pc), F32),
            pltpu.VMEM((2, nx, pieces, half, pc), BF16),
            dma((2, chunks)), dma((2,)),
            dma((2, 2)), dma((2, 2, chunks)),
            dma((2, 2)), dma((2, 2, n)),
            dma((2, 2, odd)), dma((2, 2)), dma((2, 2, chunks)),
            dma((2, pieces)), dma((2, pieces)),
            dma((2, max(nx - 1, 1), pieces)), dma((2, max(nx - 1, 1), pieces)),
            dma((2, pieces)), dma((2, pieces)),
        ],
        compiler_params=pltpu.CompilerParams(collective_id=0, has_side_effects=True),
    )(
        x, gain1.reshape(1, cols), gate1, up1, down1.reshape(chunks, w, cols),
        gain2.reshape(1, cols), gate2, up2, down2.reshape(chunks, w, cols),
    )


def solution(mesh):
    placed = (
        P("grp", "ra"),
        P("ra"),
        P("ra", "cb"),
        P("ra", "cb"),
        P("cb", "ra"),
        P("ra"),
        P("ra", "cb"),
        P("ra", "cb"),
        P("cb", "ra"),
    )
    body = functools.partial(per_device, mesh.shape["ra"], mesh.shape["cb"])
    return jax.shard_map(
        body, mesh=mesh, in_specs=placed, out_specs=P("grp", "ra"), check_vma=False
    )
```

```python
import functools

import jax
import jax.numpy as jnp
from jax import lax
from jax.experimental import pallas as pl
from jax.experimental.pallas import tpu as pltpu
from jax.sharding import PartitionSpec as P

MESH = pl.DeviceIdType.MESH
F32 = jnp.float32
BF16 = jnp.bfloat16
LAG = 4


def kernel(
    n, m, chunks, w, half, width,
    x_ref, gain1, gate1, up1, down1, gain2, gate2, up2, down2, o_ref,
    xs, normed, wgu, wdn, send, recv, hid, sq_own, sq_in, sc, acc, r1, slots,
    w_sem, d_sem, send_sem, recv_sem, sq_send, sq_recv, dir_send, rel_send, hid_recv,
    core_send, core_recv, x_send, x_recv, mid_send, mid_recv,
):
    r = lax.axis_index("ra")
    b = lax.axis_index("cb")
    k0 = lax.rem(b, 2)
    xi = lax.div(b, 2)
    nx = m // 2
    sib = xi * 2 + 1 - k0
    odd = list(range(1, n, 2))
    quarter = half // 2
    gains = (gain1, gain2)

    def along(s, d, p):
        flip = d if s == 0 else 1 - d
        return p + flip * (n - 1 - 2 * p)

    def pos(s, d):
        return along(s, d, r)

    def gate_copies(s, c):
        at = pl.ds(pl.multiple_of(c * w, w), w)
        g, u = ((gate1, up1), (gate2, up2))[s]
        return (
            pltpu.make_async_copy(g.at[:, at], wgu.at[s, c, :, pl.ds(0, w)], w_sem.at[s, c]),
            pltpu.make_async_copy(u.at[:, at], wgu.at[s, c, :, pl.ds(w, w)], w_sem.at[s, c]),
        )

    def down_copy(s):
        return pltpu.make_async_copy((down1, down2)[s], wdn.at[s], d_sem.at[s])

    for s in range(2):
        @pl.loop(0, chunks)
        def _(c):
            for copy in gate_copies(s, c):
                copy.start()
        down_copy(s).start()

    barrier = pltpu.get_barrier_semaphore()
    for o in range(1, n):
        pl.semaphore_signal(barrier, 1, device_id={"ra": lax.rem(r + o, n)}, device_id_type=MESH)
    pl.semaphore_signal(barrier, 1, device_id={"cb": sib}, device_id_type=MESH)
    for o in range(1, nx):
        pl.semaphore_signal(
            barrier, 1, device_id={"cb": lax.rem(xi + o, nx) * 2 + k0}, device_id_type=MESH
        )

    for d in range(2):
        for t in range(2):
            at = d * half + t * quarter
            xs[0, d, t] = x_ref[at:at + quarter]

    def remote(src, dst, ss, rs, where):
        return pltpu.make_async_remote_copy(
            src_ref=src, dst_ref=dst, send_sem=ss, recv_sem=rs, device_id=where, device_id_type=MESH
        )

    def sum_copy(s, d, c):
        return remote(send.at[s, d, c], recv.at[s, d, c], send_sem.at[s, d], recv_sem.at[s, d, c],
                      {"ra": along(s, d, pos(s, d) + 1)})

    def hid_copy(s, d, c, ss, q):
        ref = hid.at[s, d, c]
        return remote(ref, ref, ss, hid_recv.at[s, d, c], {"ra": along(s, d, n - 1 - q)})

    def sq_copy(s, d, p):
        return remote(sq_own.at[s, d], sq_in.at[s, d, p], sq_send.at[s, d], sq_recv.at[s, d, p],
                      {"ra": along(s, d, n - 1)})

    def core_copy(s, d):
        return remote(acc.at[s, d, 1 - k0], r1.at[s, d], core_send.at[s, d], core_recv.at[s, d],
                      {"cb": sib})

    def x_copy(s, d, o):
        ref = slots.at[s, xi, d]
        return remote(ref, ref, x_send.at[s, o - 1, d], x_recv.at[s, o - 1, d],
                      {"cb": lax.rem(xi + o, nx) * 2 + k0})

    def mid_copy(s, d):
        ref = xs.at[s + 1, d, k0]
        return remote(ref, ref, mid_send.at[s, d], mid_recv.at[s, d], {"cb": sib})

    lane = lax.broadcasted_iota(jnp.int32, (8, 128), 1)

    def norm(s, d):
        gain = gains[s][...].astype(F32)[None, :]
        packed = jnp.zeros((8, 128), F32)
        for t in range(2):
            xf = xs[s, d, t].astype(F32)
            total = jnp.sum(xf * xf, axis=1, keepdims=True)
            normed[s, d, t * quarter:(t + 1) * quarter] = (xf * gain).astype(BF16)
            for g in range(quarter // 8):
                packed = jnp.where(lane == t * (quarter // 8) + g, total[g * 8:(g + 1) * 8], packed)
        sq_own[s, d] = packed

    def greet(s, d):
        @pl.when(pos(s, d) < n - 1)
        def _():
            sq_copy(s, d, pos(s, d)).start()

    def down(s, d):
        back = n - 1 - pos(s, d)
        cuts = sorted({0, max(chunks - 5, 0), max(chunks - 2, 0), chunks})
        for lo, hi in zip(cuts, cuts[1:]):
            @pl.when((back > 0) & ((lax.rem(back, 2) == 0) | (back == n - 1)))
            def _():
                for c in range(lo, hi):
                    hid_copy(s, d, c, rel_send.at[s, d], 1).wait_recv()

            rows = jnp.concatenate([hid[s, d, c] for c in range(lo, hi)], axis=1)
            out = jnp.dot(
                rows, wdn[s, lo:hi].reshape((hi - lo) * w, wdn.shape[-1]), preferred_element_type=F32
            )
            for t in range(2):
                part = out[t * quarter:(t + 1) * quarter]
                acc[s, d, t] = part if lo == 0 else acc[s, d, t] + part

        core_copy(s, d).start()

    def pair(s, d):
        core_copy(s, d).wait_recv()
        slots[s, xi, d] = (acc[s, d, k0] + r1[s, d]).astype(BF16)
        for o in range(1, nx):
            x_copy(s, d, o).start()

    def cross(s, d):
        for o in range(1, nx):
            x_copy(s, d, o).wait_recv()
        branch = slots[s, 0, d].astype(F32)
        for o in range(1, nx):
            branch = branch + slots[s, o, d].astype(F32)
        xs[s + 1, d, k0] = (0.5 * xs[s, d, k0].astype(F32) + 0.5 * branch).astype(BF16)
        mid_copy(s, d).start()

    def finish(s, d):
        mid_copy(s, d).wait_recv()
        if s == 0:
            norm(1, d)
            greet(1, d)

    near = jnp.where(2 * r >= n, 0, 1)
    edge = (r == 0) | (r == n - 1)

    def single(s, d):
        down(s, d)
        pair(s, d)
        cross(s, d)
        finish(s, d)

    def both(s, f):
        down(s, f)
        pair(s, f)
        down(s, 1 - f)
        cross(s, f)
        pair(s, 1 - f)
        finish(s, f)
        cross(s, 1 - f)
        finish(s, 1 - f)

    for s in range(2):
        if s == 0:
            for d in range(2):
                norm(0, d)
            pl.semaphore_wait(barrier, n - 1 + nx)
            for d in range(2):
                greet(0, d)
        else:
            @pl.when(edge)
            def _():
                single(0, near)

            @pl.when(jnp.logical_not(edge))
            def _():
                both(0, near)

        @pl.loop(0, chunks + LAG * n)
        def _(i):
            if s == 1:
                @pl.when(edge & (i == LAG * (n - 1)))
                def _():
                    single(0, 1 - near)

            first = i - LAG * jnp.minimum(r, n - 1 - r)

            @pl.when((first >= 0) & (first < chunks))
            def _():
                whole = wgu.at[s, first]
                pltpu.make_async_copy(whole, whole, w_sem.at[s, first]).wait()

            for d in range(2):
                at = pos(s, d)
                c = i - LAG * at

                @pl.when((c >= 0) & (c < chunks))
                def _():
                    share = jnp.dot(normed[s, d], wgu[s, c], preferred_element_type=F32)

                    @pl.when(at == 0)
                    def _():
                        send[s, d, c] = share.astype(BF16)

                    @pl.when((at > 0) & (at < n - 1))
                    def _():
                        sum_copy(s, d, c).wait_recv()
                        send[s, d, c] = (share + recv[s, d, c].astype(F32)).astype(BF16)

                    @pl.when(at < n - 1)
                    def _():
                        sum_copy(s, d, c).start()

                    @pl.when(at == n - 1)
                    def _():
                        @pl.when(c == 0)
                        def _():
                            packed = sq_own[s, d]
                            for p in range(n - 1):
                                sq_copy(s, d, p).wait_recv()
                                packed = packed + sq_in[s, d, p]
                            packed = lax.rsqrt(packed / width + 1e-06)
                            for g in range(half // 8):
                                sc[s, d, g * 8:(g + 1) * 8] = jnp.broadcast_to(
                                    packed[:, g:g + 1], (8, 128)
                                )

                        sum_copy(s, d, c).wait_recv()
                        pre = share + recv[s, d, c].astype(F32)
                        scale = sc[s, d]
                        gate = pre[:, :w] * scale
                        up = pre[:, w:] * scale
                        hid[s, d, c] = (gate / (1.0 + jnp.exp(-gate)) * up).astype(BF16)
                        for t, q in enumerate(odd):
                            hid_copy(s, d, c, dir_send.at[s, d, t], q).start()

                back = n - 1 - at
                e = i - LAG * n

                @pl.when((lax.rem(back, 2) == 1) & (back < n - 1) & (e >= 0))
                def _():
                    hid_copy(s, d, e, rel_send.at[s, d], back + 1).wait_recv()
                    hid_copy(s, d, e, rel_send.at[s, d], back + 1).start()

        down_copy(s).wait()

    both(1, 1 - near)

    for d in range(2):
        for t in range(2):
            at = d * half + t * quarter
            o_ref[at:at + quarter] = xs[2, d, t]

    for s in range(2):
        for d in range(2):
            at = pos(s, d)

            @pl.when(at < n - 1)
            def _():
                sq_copy(s, d, 0).wait_send()
                remote(send.at[s, d], recv.at[s, d], send_sem.at[s, d], recv_sem.at[s, d, 0],
                       {"ra": along(s, d, at + 1)}).wait_send()

            ref = hid.at[s, d]

            @pl.when(at == n - 1)
            def _():
                for t, q in enumerate(odd):
                    remote(ref, ref, dir_send.at[s, d, t], hid_recv.at[s, d, 0],
                           {"ra": along(s, d, n - 1 - q)}).wait_send()

            back = n - 1 - at

            @pl.when((lax.rem(back, 2) == 1) & (back < n - 1))
            def _():
                remote(ref, ref, rel_send.at[s, d], hid_recv.at[s, d, 0],
                       {"ra": along(s, d, at - 1)}).wait_send()

            core_copy(s, d).wait_send()
            mid_copy(s, d).wait_send()
            for o in range(1, nx):
                x_copy(s, d, o).wait_send()


def per_device(n, m, x, gain1, gate1, up1, down1, gain2, gate2, up2, down2):
    rows, cols = x.shape
    ff = gate1.shape[1]
    w = 128
    chunks = -(-ff // w)
    ragged = chunks * w - ff
    if ragged:
        gate1, up1, gate2, up2 = (
            jnp.pad(a, ((0, 0), (0, ragged))) for a in (gate1, up1, gate2, up2)
        )
        down1, down2 = (jnp.pad(a, ((0, ragged), (0, 0))) for a in (down1, down2))
    half = rows // 2
    quarter = half // 2
    odd = n // 2
    nx = m // 2
    vmem = pl.BlockSpec(memory_space=pltpu.VMEM)
    hbm = pl.BlockSpec(memory_space=pl.ANY)
    dma = pltpu.SemaphoreType.DMA
    return pl.pallas_call(
        functools.partial(kernel, n, m, chunks, w, half, cols * n),
        out_shape=jax.ShapeDtypeStruct((rows, cols), BF16),
        in_specs=[vmem, vmem, hbm, hbm, hbm, vmem, hbm, hbm, hbm],
        out_specs=vmem,
        scratch_shapes=[
            pltpu.VMEM((3, 2, 2, quarter, cols), BF16),
            pltpu.VMEM((2, 2, half, cols), BF16),
            pltpu.VMEM((2, chunks, cols, 2 * w), BF16),
            pltpu.VMEM((2, chunks, w, cols), BF16),
            pltpu.VMEM((2, 2, chunks, half, 2 * w), BF16),
            pltpu.VMEM((2, 2, chunks, half, 2 * w), BF16),
            pltpu.VMEM((2, 2, chunks, half, w), BF16),
            pltpu.VMEM((2, 2, 8, 128), F32),
            pltpu.VMEM((2, 2, n, 8, 128), F32),
            pltpu.VMEM((2, 2, half, 128), F32),
            pltpu.VMEM((2, 2, 2, quarter, cols), F32),
            pltpu.VMEM((2, 2, quarter, cols), F32),
            pltpu.VMEM((2, nx, 2, quarter, cols), BF16),
            dma((2, chunks)), dma((2,)),
            dma((2, 2)), dma((2, 2, chunks)),
            dma((2, 2)), dma((2, 2, n)),
            dma((2, 2, odd)), dma((2, 2)), dma((2, 2, chunks)),
            dma((2, 2)), dma((2, 2)),
            dma((2, max(nx - 1, 1), 2)), dma((2, max(nx - 1, 1), 2)),
            dma((2, 2)), dma((2, 2)),
        ],
        compiler_params=pltpu.CompilerParams(collective_id=0, has_side_effects=True),
    )(
        x, gain1, gate1, up1, down1.reshape(chunks, w, cols),
        gain2, gate2, up2, down2.reshape(chunks, w, cols),
    )


def solution(mesh):
    placed = (
        P("grp", "ra"),
        P("ra"),
        P("ra", "cb"),
        P("ra", "cb"),
        P("cb", "ra"),
        P("ra"),
        P("ra", "cb"),
        P("ra", "cb"),
        P("cb", "ra"),
    )
    body = functools.partial(per_device, mesh.shape["ra"], mesh.shape["cb"])
    return jax.shard_map(
        body, mesh=mesh, in_specs=placed, out_specs=P("grp", "ra"), check_vma=False
    )
```
